256 devices in a mesh: rep: 2 (over z_hi), fs: 16 (over z_lo, y), tp: 8 (over x, core).
Axes of the slice: x: 4, y: 4, z: 8 (z_hi: 2, z_lo: 4; z = z_hi * 4 + z_lo), core: 2. Of those that a mesh axis runs over, the one named last changes fastest.
Arguments:
- tokens: bfloat16 [65536, 2048], P(('rep', 'fs', 'tp')), may hold values from -6 to 6
- norm_gain: float32 [2048], replicated, may hold values from 0.1 to 1.9
- gate_weight: float32 [2048, 5120], P('fs', 'tp'), may hold values from -0.125 to 0.125
- gate_scale: float32 [5120], P('tp'), may hold values from 0.1 to 1.9
- up_weight: float32 [2048, 5120], P('fs', 'tp'), may hold values from -0.125 to 0.125
- up_scale: float32 [5120], P('tp'), may hold values from 0.1 to 1.9
- down_weight: float32 [5120, 2048], P('tp', 'fs'), may hold values from -0.078125 to 0.078125
- down_scale: float32 [2048], replicated, may hold values from 0.1 to 1.9
Outputs:
- mixed: bfloat16 [65536, 2048], P(('rep', 'fs', 'tp'))
The draws below stay inside these ranges and needn't reach their ends.
All inputs are finite; a program needn't handle non-finite values.
Results may differ from the reference program's by a relative error of at most 0.013.
Values may be sent and summed in bfloat16 or wider, within the bound.
No kernel may reach another device: no remote copies, remote signals or barrier semaphores. Data moves between devices by JAX's collectives and lax.ppermute only.
A program may use at most 128 MiB of HBM per device.

```python
import jax
import jax.numpy as jnp
from jax import lax

D = 2048
FF = 5120
TOK_DEV = 256
TOKENS = 65536
N_TP = 8


def steps_of(key, shape, cuts, low, top_value):
    def one(position, blocks):
        steps = jax.random.uniform(jax.random.fold_in(jax.random.fold_in(key, 6), position), (blocks,), jnp.float32, low / len(cuts), top_value / len(cuts))
        return jnp.repeat(jnp.exp(steps), shape[position] // blocks).reshape((-1,) + (1,) * (len(shape) - position - 1))

    level = one(*cuts[0])
    for cut in cuts[1:]:
        level = level * one(*cut)
    return level


def bell_draw(key, extent, spread, limit, pieces=(), kind=jnp.bfloat16):
    drawn = spread * jax.random.normal(key, extent, jnp.float32)
    if pieces:
        drawn = drawn * steps_of(key, extent, pieces, -0.22, 0.18)
    return jnp.clip(drawn, -limit, limit).astype(kind)


def setup_inputs(seed: int = 0) -> dict:
    splits = jax.random.split(jax.random.key(seed), 9)
    return {
        "tokens": bell_draw(splits[0], (TOKENS, D), 1.0, 6.0, ((0, 256),)),
        "norm_gain": jnp.clip(1.0 + 0.18 * jax.random.normal(splits[1], (D,), jnp.float32), 0.1, 1.9),
        "gate_weight": bell_draw(splits[2], (D, FF), D ** -0.5, 0.125, ((0, 16), (1, 8)), jnp.float32),
        "gate_scale": jnp.clip(1.0 + 0.18 * jax.random.normal(splits[3], (FF,), jnp.float32), 0.1, 1.9),
        "up_weight": bell_draw(splits[4], (D, FF), D ** -0.5, 0.125, ((0, 16), (1, 8)), jnp.float32),
        "up_scale": jnp.clip(1.0 + 0.18 * jax.random.normal(splits[5], (FF,), jnp.float32), 0.1, 1.9),
        "down_weight": bell_draw(splits[6], (FF, D), FF ** -0.5, 0.078125, ((0, 8), (1, 16)), jnp.float32),
        "down_scale": jnp.clip(1.0 + 0.18 * jax.random.normal(splits[7], (D,), jnp.float32), 0.1, 1.9),
    }


EPS_VALUE = 1e-06

def normalize(token_rows, norm_gain):
    values = token_rows.astype(jnp.float32)
    inverse = lax.rsqrt(lax.optimization_barrier(jnp.mean(values * values, axis=-1, keepdims=True)) + EPS_VALUE)
    return (values * inverse * norm_gain).astype(jnp.bfloat16)

def reference(tokens, norm_gain, gate_weight, gate_scale, up_weight, up_scale, down_weight, down_scale):
    gate_bf = gate_weight.astype(jnp.bfloat16)
    up_bf = up_weight.astype(jnp.bfloat16)
    down_bf = down_weight.astype(jnp.bfloat16)
    width_tp = FF // N_TP
    down_blocks = down_bf.reshape(N_TP, width_tp, D)
    group_rows = TOK_DEV * N_TP

    def one_group(token_rows):
        normed = normalize(token_rows, norm_gain)
        gate_pre = jnp.dot(normed, gate_bf, preferred_element_type=jnp.float32) * gate_scale
        up_pre = jnp.dot(normed, up_bf, preferred_element_type=jnp.float32) * up_scale
        hidden = (jax.nn.silu(gate_pre) * up_pre).astype(jnp.bfloat16)
        total = jnp.zeros((group_rows, D), jnp.float32)
        for tp_block in range(N_TP):
            columns = hidden[:, tp_block * width_tp:(tp_block + 1) * width_tp]
            partial_value = (jnp.dot(columns, down_blocks[tp_block], preferred_element_type=jnp.float32) * down_scale).astype(jnp.bfloat16)
            partial_value = lax.optimization_barrier(partial_value)
            total = total + partial_value.astype(jnp.float32)
        return total.astype(jnp.bfloat16)
    grouped = tokens.reshape(TOKENS // group_rows, group_rows, D)
    return lax.map(one_group, grouped).reshape(TOKENS, D)
```

```python
import jax
import jax.numpy as jnp
from jax import lax
from jax.experimental import pallas as pl
from jax.experimental.pallas import tpu as pltpu
from jax.sharding import PartitionSpec as P

EPS_VALUE = 1e-06
AXES = ("rep", "fs", "tp")
NY = 4
ORDER = (0, 1, -1, 2)
F32 = jnp.float32
BF16 = jnp.bfloat16


class Torus:
    def __init__(self, mesh):
        self.rep, self.fs, self.tp = (mesh.shape[a] for a in AXES)
        self.nx, self.nzl = self.tp // 2, self.fs // NY
        self.nz = self.rep * self.nzl

    def number(self, x, y, z, c):
        x, y, z, c = x % self.nx, y % NY, z % self.nz, c % 2
        return ((z // self.nzl) * self.fs + (z % self.nzl) * NY + y) * self.tp + 2 * x + c

    def perm(self, source):
        pairs = []
        for x in range(self.nx):
            for y in range(NY):
                for z in range(self.nz):
                    for c in range(2):
                        pairs.append((self.number(*source(x, y, z, c)), self.number(x, y, z, c)))
        return pairs

    def take(self, value, dx=0, dy=0, dz=0, dc=0):
        return lax.ppermute(value, AXES, self.perm(lambda x, y, z, c: (x + dx, y + dy, z + dz, c + dc)))

    def take_z2(self, value):
        return lax.ppermute(
            value, AXES, self.perm(lambda x, y, z, c: (x, y, z + (2 if z % 2 == 0 else -2), c))
        )


def normalize(token_rows, norm_gain):
    values = token_rows.astype(F32)
    inverse = lax.rsqrt(jnp.mean(values * values, axis=-1, keepdims=True) + EPS_VALUE)
    return (values * inverse * norm_gain).astype(BF16)


def ffn_kernel(ids_a, ids_b, *refs, blocks, parts, wide, hid):
    toks, refs = refs[: blocks * parts], refs[blocks * parts :]
    a_refs, b_refs, gs, us, outs = refs[:5], refs[5:10], refs[10], refs[11], refs[12:]
    tail = 2 * hid - wide

    def columns(tok, ids, at, count):
        cols = []
        for k in range(count):
            where = pl.ds(pl.multiple_of(ids[at + k] * 128, 128), 128)
            rows = [t[:, where] for t in tok]
            cols.append(rows[0] if len(rows) == 1 else jnp.concatenate(rows, axis=0))
        return jnp.concatenate(cols, axis=1)

    def product(tok, ids, weights, cols):
        total, at = None, 0
        for w in weights:
            count = w.shape[0] // 128
            term = jnp.dot(columns(tok, ids, at, count), w[:, cols], preferred_element_type=F32)
            total = term if total is None else total + term
            at += count
        return total

    for n in range(blocks):
        tok = toks[n * parts : (n + 1) * parts]
        left = product(tok, ids_a, a_refs, slice(0, wide))
        right = product(tok, ids_b, b_refs, slice(0, tail))
        gate = left[:, :hid] * gs[...]
        up = jnp.concatenate([left[:, hid:], right], axis=1) * us[...]
        hidden = (gate / (1.0 + jnp.exp(-gate)) * up).astype(BF16)
        at = 0
        for w in b_refs:
            part = lax.dot_general(
                hidden, w[:, tail:], (((1,), (1,)), ((), ())), preferred_element_type=F32
            ).astype(BF16)
            for k in range(w.shape[0] // 128):
                where = pl.ds(pl.multiple_of(ids_b[at + k] * 128, 128), 128)
                outs[n][:, where] = part[:, k * 128 : (k + 1) * 128]
            at += w.shape[0] // 128


def ffn(ids_a, ids_b, blocks, a_parts, b_parts, gs, us):
    parts = len(blocks[0])
    flat = [t for b in blocks for t in b]
    width = flat[0].shape[1]
    rows = sum(t.shape[0] for t in blocks[0])
    wide, hid = a_parts[0].shape[1], gs.shape[1]
    smem = pl.BlockSpec(memory_space=pltpu.SMEM)
    vmem = pl.BlockSpec(memory_space=pltpu.VMEM)
    count = len(blocks)
    return pl.pallas_call(
        lambda *r: ffn_kernel(*r, blocks=count, parts=parts, wide=wide, hid=hid),
        out_shape=[jax.ShapeDtypeStruct((rows, width), BF16)] * count,
        in_specs=[smem, smem] + [vmem] * (len(flat) + 12),
        out_specs=[vmem] * count,
        compiler_params=pltpu.CompilerParams(vmem_limit_bytes=40 * 2**20),
        cost_estimate=pl.CostEstimate(
            flops=6 * count * rows * width * hid, bytes_accessed=2**20, transcendentals=count * rows * hid
        ),
        name="ffn",
    )(ids_a, ids_b, *flat, *a_parts, *b_parts, gs, us)


def build(mesh):
    torus = Torus(mesh)
    take = torus.take

    def body(tokens, norm_gain, gate_weight, gate_scale, up_weight, up_scale, down_weight, down_scale):
        hid = gate_weight.shape[1]
        wide = (2 * hid * 8 // 10) // 256 * 256
        split = wide - hid
        gate_bf, up_bf, down_t = gate_weight.astype(BF16), up_weight.astype(BF16), down_weight.astype(BF16).T
        a = jnp.concatenate([gate_bf, up_bf[:, :split]], axis=1)
        b = jnp.concatenate([up_bf[:, split:], down_t], axis=1)

        fs = lax.axis_index("fs")
        zl, y = fs // NY, fs % NY
        piece = lambda dy, dz: ((zl + dz) % torus.nzl) * NY + (y + dy) % NY
        ids_a = jnp.stack([piece(dy, dz) for dy in ORDER for dz in ORDER]).astype(jnp.int32)
        ids_b = jnp.stack([piece(dy, dz) for dz in ORDER for dy in ORDER]).astype(jnp.int32)

        a4 = jnp.concatenate([a, take(a, dz=1), take(a, dz=-1), torus.take_z2(a)], axis=0)
        b4 = jnp.concatenate([b, take(b, dy=1), take(b, dy=-1), take(b, dy=2)], axis=0)
        normed = normalize(tokens, norm_gain)
        half = normed.shape[0] // 2
        t_p, t_m = take(normed, dx=1), take(normed, dx=-1)
        a_p, a_m = take(a4, dy=1), take(a4, dy=-1)
        b_p, b_m = take(b4, dz=1), take(b4, dz=-1)
        h2 = a4.shape[0] // 2
        t_2 = (take(t_m[:half], dx=-1), take(t_p[half:], dx=1))
        a_parts = (a4, a_p, a_m, take(a_p[:h2], dy=1), take(a_m[h2:], dy=-1))
        b_parts = (b4, b_p, b_m, take(b_p[:h2], dz=1), take(b_m[h2:], dz=-1))
        other = lambda ts: tuple(take(t, dc=1) for t in ts)

        gs, us = gate_scale[None, :], up_scale[None, :]
        run = lambda *blocks: ffn(ids_a, ids_b, blocks, a_parts, b_parts, gs, us)
        add = lambda *vs: sum(v.astype(F32) for v in vs)

        def chip(ts):
            theirs, mine = run(other(ts), ts)
            return mine, take(theirs, dc=1)

        far = chip(t_2)
        far = add(*far).astype(BF16)
        via_m, via_p = take(far[:half], dx=-1), take(far[half:], dx=1)
        right = add(*chip((t_p,)))
        left = add(*chip((t_m,)))
        r1 = take(right[half:].astype(BF16), dx=-1)
        l0 = take(left[:half].astype(BF16), dx=1)
        own = add(*chip((normed,)))
        r0 = take((right[:half] + via_m.astype(F32)).astype(BF16), dx=-1)
        l1 = take((left[half:] + via_p.astype(F32)).astype(BF16), dx=1)
        total = own + jnp.concatenate([add(r0, l0), add(r1, l1)], axis=0)
        return (total * down_scale).astype(BF16)

    return body


def solution(mesh):
    return jax.shard_map(
        build(mesh),
        mesh=mesh,
        in_specs=(
            P(AXES, None),
            P(),
            P("fs", "tp"),
            P("tp"),
            P("fs", "tp"),
            P("tp"),
            P("tp", "fs"),
            P(),
        ),
        out_specs=P(AXES, None),
        check_vma=False,
    )
```
